32 devices in a mesh: sp: 8 (over z, x), tp: 4 (over y, core).
Axes of the slice: x: 2, y: 2, z: 4, core: 2. Of those that a mesh axis runs over, the one named last changes fastest.
Arguments:
- tokens: bfloat16 [2048, 2048], P('sp', 'tp'), may hold values from -6 to 6
- segments: int32 [2048], P('sp'), may hold values from 0 to 3, never falling along the last dimension, each value on 1 to 1024 neighbouring positions
- in_gain: float32 [2, 2048], replicated, may hold values from 0.1 to 1.9
- w_value: bfloat16 [2, 2048, 1024], P(None, 'sp', 'tp'), may hold values from -0.125 to 0.125
- w_gate: bfloat16 [2, 2048, 1024], P(None, 'sp', 'tp'), may hold values from -0.125 to 0.125
- conv_taps: float32 [2, 129, 1024], P(None, None, 'tp'), may hold values from -4 to 4, as said below
- norm_gain: float32 [2, 1024], P(None, 'tp'), may hold values from 0.1 to 1.9
- w_out: bfloat16 [2, 1024, 2048], P(None, 'tp', 'sp'), may hold values from -0.1875 to 0.1875
Outputs:
- mixed: bfloat16 [2048, 2048], P('sp', 'tp')
The draws below stay inside these ranges and needn't reach their ends.
Inputs may be any that keep to these rules, and one draw needn't show every extreme that they name: `segments`: document numbers never fall along the sequence; each document has 1 to 1024 positions, one has exactly 1024. `conv_taps`: real-valued taps.
All inputs are finite; a program needn't handle non-finite values.
Results may differ from the reference program's by a relative error of at most 0.014.
Values may be sent and summed in bfloat16 or wider, within the bound.
A program may use at most 64 MiB of HBM per device.

```python
import math
import jax
import jax.numpy as jnp
import numpy as np
from jax import lax

D = 2048
CF = 1024
KW = 129
LAYERS = 2
TOKENS = 2048
CF_DEV = 256
DOCS = 4
DOC_MOST = 1024
N_TP = 4


def draw_conv_taps(key, part):
    first, second = jax.random.split(key, 2)
    group_scale = jnp.exp(jax.random.uniform(first, (8,), jnp.float32, jnp.log(0.3), jnp.log(3.0)))
    channel_scale = jnp.repeat(group_scale, CF // 8)
    base = jnp.clip(jax.random.normal(second, (LAYERS, KW, CF), jnp.float32), -4.0, 4.0)
    return (base * channel_scale * KW ** (-0.5)).astype(jnp.float32)


def block_scale(stream_key, extent, cuts, low, high):
    level, own = 1.0, jax.random.fold_in(stream_key, 6)
    for dim, parts in cuts:
        heights = jnp.exp(jax.random.uniform(jax.random.fold_in(own, dim), (parts,), jnp.float32, low / len(cuts), high / len(cuts)))
        level = level * jnp.repeat(heights, extent[dim] // parts).reshape([-1 if axis == dim else 1 for axis in range(len(extent))])
    return level


def length_profile(number_of, total, bound, lean):
    weights = [(1 << 20) // math.isqrt(grade ** lean) + 1 for grade in range(2, number_of + 1)]
    rest, given = total - bound - (number_of - 1), [1] * (number_of - 1)
    while rest > 0:
        candidates = [i for i in range(number_of - 1) if given[i] < bound]
        whole, remaining = sum([weights[i] for i in candidates]), rest
        for i in candidates:
            more = min(bound - given[i], max(1, remaining * weights[i] // whole), rest)
            given[i] = given[i] + more
            rest = rest - more
    return np.array([bound] + given)


def ragged(own_key, number_of, total, most, slope):
    if number_of == 2:
        one = jax.random.randint(own_key, (), max(1, total - most), min(most, total - 1) + 1)
        return jnp.stack([one, total - one])
    lengths = jnp.asarray(length_profile(number_of, total, most, slope), jnp.int32)
    couples = (number_of - 1) // 2
    giver, taker = lengths[1:1 + 2 * couples:2], lengths[2:2 + 2 * couples:2]
    margin = jnp.minimum(giver - 1, most - taker)
    moved = jax.random.randint(jax.random.fold_in(own_key, 1), (couples,), 0, 1 << 20) % (margin + 1)
    lengths = lengths.at[1:1 + 2 * couples:2].set(giver - moved).at[2:2 + 2 * couples:2].set(taker + moved)
    return lengths[jax.random.permutation(jax.random.fold_in(own_key, 2), number_of)]


def bell_draw(rng, extent, spread, reach, shards=(), dtype=jnp.bfloat16):
    drawn = spread * jax.random.normal(rng, extent, jnp.float32)
    if shards:
        drawn = drawn * block_scale(rng, extent, shards, -0.22, 0.18)
    return jnp.clip(drawn, -reach, reach).astype(dtype)


def setup_inputs(seed: int = 0) -> dict:
    arg_keys = jax.random.split(jax.random.key(seed), 9)
    tokens = bell_draw(arg_keys[0], (TOKENS, D), 1.0, 6.0, ((0, 8), (1, 4)))
    segments = jnp.searchsorted(jnp.cumsum(ragged(arg_keys[1], DOCS, TOKENS, DOC_MOST, 2)), jnp.arange(TOKENS), side="right").astype(jnp.int32)
    in_gain = jnp.clip(1.0 + 0.18 * jax.random.normal(arg_keys[2], (LAYERS, D), jnp.float32), 0.1, 1.9)
    w_value = bell_draw(arg_keys[3], (LAYERS, D, CF), D ** -0.5, 0.125, ((1, 8), (2, 4)))
    w_gate = bell_draw(arg_keys[4], (LAYERS, D, CF), D ** -0.5, 0.125, ((1, 8), (2, 4)))
    conv_taps = draw_conv_taps(jax.random.fold_in(arg_keys[8], 71), 0)
    norm_gain = jnp.clip(1.0 + 0.18 * jax.random.normal(arg_keys[6], (LAYERS, CF), jnp.float32), 0.1, 1.9)
    w_out = bell_draw(arg_keys[7], (LAYERS, CF, D), CF ** -0.5, 0.1875, ((1, 4), (2, 8)))
    return {"tokens": tokens, "segments": segments, "in_gain": in_gain, "w_value": w_value, "w_gate": w_gate, "conv_taps": conv_taps, "norm_gain": norm_gain, "w_out": w_out}


EPSILON = 0.01

def rms_rows(stream, gain):
    wide_vals = stream.astype(jnp.float32)
    scale = lax.rsqrt(lax.optimization_barrier(jnp.mean(wide_vals * wide_vals, axis=-1, keepdims=True)) + EPSILON)
    return (wide_vals * scale * gain).astype(jnp.bfloat16)

def reference(tokens, segments, in_gain, w_value, w_gate, conv_taps, norm_gain, w_out):
    fringe = (KW - 1) // 2
    seg_pad = jnp.pad(segments, (fringe, fringe), constant_values=-1)
    stream = tokens
    for layer_idx in range(LAYERS):
        normed = rms_rows(stream, in_gain[layer_idx])
        value_pre = jnp.dot(normed, w_value[layer_idx], preferred_element_type=jnp.float32)
        gate_pre = jnp.dot(normed, w_gate[layer_idx], preferred_element_type=jnp.float32)
        gated = (value_pre * jax.nn.sigmoid(gate_pre)).astype(jnp.bfloat16)
        padded = jnp.pad(gated.astype(jnp.float32), ((fringe, fringe), (0, 0)))
        tap_table = conv_taps[layer_idx]

        def add_tap(shift_idx, running):
            shift_idx = jnp.asarray(shift_idx).astype(jnp.int32)
            window = lax.dynamic_slice_in_dim(padded, shift_idx, TOKENS, 0)
            same_doc = lax.dynamic_slice_in_dim(seg_pad, shift_idx, TOKENS, 0) == segments
            tap_row = lax.dynamic_slice_in_dim(tap_table, shift_idx, 1, 0)
            return running + jnp.where(same_doc[:, None], window * tap_row, jnp.float32(0.0))
        conv = lax.fori_loop(0, KW, add_tap, jnp.zeros((TOKENS, CF), jnp.float32))
        row_mean = lax.optimization_barrier(jnp.mean(conv, axis=-1, keepdims=True))
        centred = conv - row_mean
        row_var = lax.optimization_barrier(jnp.mean(centred * centred, axis=-1, keepdims=True))
        activated = jax.nn.silu(centred * lax.rsqrt(row_var + EPSILON) * norm_gain[layer_idx]).astype(jnp.bfloat16)
        out_weight = w_out[layer_idx]

        def add_block(block_idx, running):
            first = (jnp.asarray(block_idx) * CF_DEV).astype(jnp.int32)
            columns = lax.dynamic_slice_in_dim(activated, first, CF_DEV, 1)
            weight_rows = lax.dynamic_slice_in_dim(out_weight, first, CF_DEV, 0)
            partial_value = jnp.dot(columns, weight_rows, preferred_element_type=jnp.float32)
            return running + lax.optimization_barrier(partial_value.astype(jnp.bfloat16)).astype(jnp.float32)
        summed = lax.fori_loop(0, N_TP, add_block, jnp.zeros((TOKENS, D), jnp.float32))
        stream = (stream.astype(jnp.float32) + summed).astype(jnp.bfloat16)
    return stream
```

```python
import functools

import jax
import jax.numpy as jnp
from jax import lax
from jax.experimental import pallas as pl
from jax.experimental.pallas import tpu as pltpu
from jax.sharding import PartitionSpec as P

EPSILON = 0.01
LANES = 128
PAIR = 2
RELAY_MOST = 8
DETOUR = {1: 1, 2: 2, 4: 1}
F32 = jnp.float32
BF16 = jnp.bfloat16
MESH = pl.DeviceIdType.MESH


def remote(src, dst, send, recv, device):
    return pltpu.make_async_remote_copy(
        src_ref=src, dst_ref=dst, send_sem=send, recv_sem=recv, device_id=device, device_id_type=MESH
    )


def guarded(cond, act):
    if cond is None:
        act()
    else:
        pl.when(cond)(act)


def kernel(
    cfg, tok, seg, gain_in_hbm, wv, wg, wo, taps_hbm, gain_norm_hbm, out,
    stream, normed, gv, go_w, vacc, gacc, gbf, halo, xbuf, segw, segraw, segn, conv, act, stat, part,
    first, pair, far, own, gain_in, gain_norm, taps,
    local_sem, w_recv, w_send, tok_recv, tok_send, sib_send, seg_send, seg_recv,
    halo_send, halo_recv, stat_send, stat_recv, first_send, first_recv, far_send, far_recv, back_recv,
):
    n_sp, n_tp, layers, kw, gather = cfg
    fringe = (kw - 1) // 2
    rows, width = tok.shape
    tiles = xbuf.shape[0]
    chan = tiles * LANES
    line, half = n_sp // PAIR, n_tp // PAIR
    s, t = lax.axis_index("sp"), lax.axis_index("tp")
    z, x = s // PAIR, lax.rem(s, PAIR)
    h, c = t // PAIR, lax.rem(t, PAIR)
    x_next = z * PAIR + (1 - x)
    sib = h * PAIR + (1 - c)
    mats = 3
    chunk = rows // 2
    depth = min(wv.shape[1], width)
    blocks_in = n_tp * width // depth
    cols = go_w.shape[-1]
    each = width // cols

    sends = []

    def go(copy, cond=None):
        guarded(cond, copy.start)
        sends.append((copy, cond))

    def place(block):
        return (block % PAIR) * line + block // PAIR if gather else block

    def slot(p, zo, xo):
        layer, mat = p // mats, p % mats
        pos = xo * line + zo
        if mat == 2:
            return go_w.at[layer, pos]
        return gv.at[layer, mat, pl.ds(pl.multiple_of(pos * depth, depth), depth)]

    local = []

    def fetch(src, dst):
        copy = pltpu.make_async_copy(src, dst, local_sem.at[len(local)])
        copy.start()
        local.append(copy)
        return copy

    own_copies = []
    for p in range(layers * mats):
        src = (wv, wg, wo)[p % mats].at[p // mats]
        if gather:
            dst = slot(p, z, x)
        else:
            dst = go_w.at[p // mats] if p % mats == 2 else gv.at[p // mats, p % mats]
        own_copies.append((src, dst))
    weight_in = [fetch(*own_copies[0]), fetch(*own_copies[1])]
    tok_in = fetch(tok, stream.at[0, t])
    seg_in = fetch(seg, segraw)
    weight_in += [fetch(*pair_) for pair_ in own_copies[2:]]
    rest_in = [fetch(gain_in_hbm, gain_in), fetch(gain_norm_hbm, gain_norm), fetch(taps_hbm, taps)]

    barrier = pltpu.get_barrier_semaphore()
    prev_s, next_s = jnp.maximum(s - 1, 0), jnp.minimum(s + 1, n_sp - 1)

    def greet(device, cond=None):
        guarded(cond, lambda: pl.semaphore_signal(barrier, inc=1, device_id=device, device_id_type=MESH))

    for d in range(1, n_tp):
        greet({"tp": lax.rem(t + d, n_tp)})
    peers = n_tp - 1
    greet({"sp": prev_s}, s > 0)
    greet({"sp": next_s}, s < n_sp - 1)
    peers = peers + jnp.where(s > 0, 1, 0) + jnp.where(s < n_sp - 1, 1, 0)
    if gather:
        up = {"sp": jnp.minimum(s + PAIR, n_sp - 1)}
        down = {"sp": jnp.maximum(s - PAIR, 0)}
        side = {"sp": x_next}
        greet(up, z < line - 1)
        greet(down, z > 0)
        greet(side)
        peers = peers + 1 + jnp.where(z < line - 1, 1, 0) + jnp.where(z > 0, 1, 0)
    pl.semaphore_wait(barrier, peers)

    def push(p, kind, zo, xo, device, cond):
        block = slot(p, zo, xo)
        go(remote(block, block, w_send.at[p, kind], w_recv.at[p, xo * line + zo], device), cond)

    def landed(p, zo, xo, cond):
        block = slot(p, zo, xo)
        guarded(cond, remote(block, block, w_send.at[p, 0], w_recv.at[p, xo * line + zo], {"sp": x_next}).wait_recv)

    def own_z(p):
        if gather:
            push(p, 0, z, x, up, z < line - 1)
            push(p, 1, z, x, down, z > 0)

    def own_x(p):
        if gather:
            push(p, 2, z, x, side, None)

    def relay(p, d):
        if not gather or d >= line:
            return
        for sign in (1, -1):
            zo = z - sign * d
            here = (zo >= 0) if sign > 0 else (zo < line)
            safe = jnp.clip(zo, 0, line - 1)
            landed(p, safe, x, here)
            k = 3 + (0 if sign > 0 else 1) + 4 * (d - 1)
            onward = (z < line - 1) if sign > 0 else (z > 0)
            push(p, k, safe, x, up if sign > 0 else down, jnp.logical_and(here, onward))
            cross = here
            if p in DETOUR:
                cross = jnp.logical_and(here, safe != DETOUR[p])
            push(p, k + 2, safe, x, side, cross)

    def detour(p, d):
        if not gather or p not in DETOUR or d >= line:
            return
        zo = DETOUR[p]
        k = 3 + 4 * (line - 1)
        if d == 0:
            landed(p, zo, 1 - x, z == zo)
            push(p, k, zo, 1 - x, up, jnp.logical_and(z == zo, z < line - 1))
            push(p, k + 1, zo, 1 - x, down, jnp.logical_and(z == zo, z > 0))
        else:
            landed(p, zo, 1 - x, jnp.logical_or(z == zo + d, z == zo - d))
            push(p, k + 2 * d, zo, 1 - x, up, jnp.logical_and(z == zo + d, z < line - 1))
            push(p, k + 2 * d + 1, zo, 1 - x, down, jnp.logical_and(z == zo - d, z > 0))

    def settle(p):
        if not gather:
            return
        for d in range(line):
            for sign in ((1,) if d == 0 else (1, -1)):
                zo = z - sign * d
                safe = jnp.clip(zo, 0, line - 1)
                cond = None if d == 0 else ((zo >= 0) if sign > 0 else (zo < line))
                if p in DETOUR:
                    differs = safe != DETOUR[p]
                    cond = differs if cond is None else jnp.logical_and(cond, differs)
                landed(p, safe, 1 - x, cond)

    weight_in[0].wait()
    own_z(0)
    own_x(0)
    weight_in[1].wait()
    own_z(1)
    own_x(1)
    tok_in.wait()
    for d in range(1, half):
        go(remote(stream.at[0, t], stream.at[0, t], tok_send.at[d], tok_recv.at[t], {"tp": lax.rem(h + d, half) * PAIR + c}))
    go(remote(stream.at[0, t], stream.at[0, t], sib_send.at[0, 0], tok_recv.at[t], {"tp": sib}))
    seg_in.wait()

    def seg_copy(side_):
        return remote(segraw, segn.at[side_], seg_send.at[side_], seg_recv.at[side_], {"sp": prev_s if side_ else next_s})

    go(seg_copy(0), s < n_sp - 1)
    go(seg_copy(1), s > 0)

    def column(row):
        return jnp.transpose(jnp.broadcast_to(row.astype(F32), (LANES, LANES)))

    for i in range(rows // LANES):
        segw[pl.ds(fringe + i * LANES, LANES), :] = column(segraw[i : i + 1, :])

    relay(0, 1)
    relay(1, 1)
    for copy in weight_in[2:] + rest_in:
        copy.wait()
    for d in range(1, half):
        origin = lax.rem(h + half - d, half) * PAIR + c
        block = stream.at[0, origin]
        remote(block, block, tok_send.at[d], tok_recv.at[origin], {"tp": sib}).wait_recv()
        go(remote(block, block, sib_send.at[0, d], tok_recv.at[origin], {"tp": sib}))
    relay(0, 2)
    relay(1, 2)
    detour(1, 0)
    for d in range(half):
        origin = lax.rem(h + half - d, half) * PAIR + (1 - c)
        block = stream.at[0, origin]
        remote(block, block, sib_send.at[0, 0], tok_recv.at[origin], {"tp": sib}).wait_recv()
    guarded(s > 0, seg_copy(0).wait_recv)
    guarded(s < n_sp - 1, seg_copy(1).wait_recv)

    @pl.when(s > 0)
    def _():
        segw[pl.ds(0, fringe), :] = column(segn[0, rows // LANES - 1 : rows // LANES, :])[LANES - fringe :]

    @pl.when(s == 0)
    def _():
        segw[pl.ds(0, fringe), :] = jnp.full((fringe, LANES), -1.0, F32)

    @pl.when(s < n_sp - 1)
    def _():
        segw[pl.ds(fringe + rows, fringe), :] = column(segn[1, 0:1, :])[:fringe]

    @pl.when(s == n_sp - 1)
    def _():
        segw[pl.ds(fringe + rows, fringe), :] = jnp.full((fringe, LANES), -1.0, F32)

    spans = ((fringe, chunk),), ((0, fringe), (rows - fringe, fringe))

    for layer in range(layers):
        last = layer == layers - 1
        base_p = layer * mats

        def norm_step(i, _):
            at = pl.ds(pl.multiple_of(i * 32, 32), 32)
            total = jnp.zeros((32, 1), F32)
            for j in range(n_tp):
                v = stream[layer, j, at, :].astype(F32)
                total = total + jnp.sum(v * v, axis=-1, keepdims=True)
            scale = lax.rsqrt(total / (n_tp * width) + EPSILON)
            for b in range(blocks_in):
                j, lo = b * depth // width, b * depth % width
                v = stream[layer, j, at, lo : lo + depth].astype(F32)
                gain = gain_in[layer : layer + 1, b * depth : (b + 1) * depth]
                to = place(b) * depth
                normed[at, to : to + depth] = (v * scale * gain).astype(BF16)
            return 0

        lax.fori_loop(0, rows // 32, norm_step, 0)
        if layer == 0:
            relay(0, 3)
            relay(1, 3)
            detour(1, 1)
            detour(1, 2)
            own_z(2)

        size = n_tp * width // 2
        near = pl.multiple_of(x * size, size) if gather else 0
        away = pl.multiple_of((1 - x) * size, size) if gather else size
        a = normed[:, pl.ds(near, size)]
        vacc[...] = jnp.dot(a, gv[layer, 0, pl.ds(near, size), :], preferred_element_type=F32)
        gacc[...] = jnp.dot(a, gv[layer, 1, pl.ds(near, size), :], preferred_element_type=F32)
        settle(base_p)
        settle(base_p + 1)
        a = normed[:, pl.ds(away, size)]
        vacc[...] += jnp.dot(a, gv[layer, 0, pl.ds(away, size), :], preferred_element_type=F32)
        gacc[...] += jnp.dot(a, gv[layer, 1, pl.ds(away, size), :], preferred_element_type=F32)

        def gate_step(i, _):
            at = pl.ds(pl.multiple_of(i * 32, 32), 32)
            gated = (vacc[at, :] * jax.nn.sigmoid(gacc[at, :])).astype(BF16)
            gbf[layer, at, :] = gated
            wide = gated.astype(F32)
            to = pl.ds(pl.multiple_of(fringe + i * 32, 32), 32)
            for j in range(tiles):
                xbuf[j, to, :] = wide[:, j * LANES : (j + 1) * LANES]
            return 0

        lax.fori_loop(0, rows // 32, gate_step, 0)

        def halo_copy(side_):
            lo = 0 if side_ else rows - fringe
            return remote(
                gbf.at[layer, pl.ds(lo, fringe)], halo.at[layer, side_], halo_send.at[layer, side_],
                halo_recv.at[layer, side_], {"sp": prev_s if side_ else next_s},
            )

        go(halo_copy(0), s < n_sp - 1)
        go(halo_copy(1), s > 0)
        if layer == 0:
            own_x(2)
            relay(2, 1)
        if not last:
            own_z(base_p + 3)

        def conv_span(start, put):
            base = pl.multiple_of(start, fringe)
            here = [segw[pl.ds(base + fringe + 8 * m, 8), :] for m in range(8)]
            acc = [[jnp.zeros((8, LANES), F32) for _ in range(tiles)] for _ in range(8)]
            for shift in range(8):
                most = (kw - 1 - shift) // 8
                for n in range(most + 8):
                    at = pl.ds(base + 8 * n + shift, 8)
                    docs = segw[at, :]
                    data = [xbuf[j, at, :] for j in range(tiles)]
                    for m in range(8):
                        if 0 <= n - m <= most:
                            k = 8 * (n - m) + shift
                            same = docs == here[m]
                            for j in range(tiles):
                                tap = taps[k, layer : layer + 1, j * LANES : (j + 1) * LANES]
                                acc[m][j] = acc[m][j] + jnp.where(same, data[j] * tap, 0.0)
            lane = lax.broadcasted_iota(jnp.int32, (8, LANES), 1)
            for m in range(8):
                mean = sum(jnp.sum(v, axis=-1, keepdims=True) for v in acc[m]) / chan
                square = sum(jnp.sum((v - mean) * (v - mean), axis=-1, keepdims=True) for v in acc[m])
                at = pl.ds(put + 8 * m, 8)
                for j in range(tiles):
                    conv[at, j * LANES : (j + 1) * LANES] = acc[m][j]
                part[at, :] = jnp.where(lane == 0, mean, square)

        def send_stats(q):
            stat[layer, q, t] = jnp.transpose(part[pl.ds(q * chunk, chunk), :])[:8]
            for d in range(1, n_tp):
                go(remote(stat.at[layer, q, t], stat.at[layer, q, t], stat_send.at[layer, q, d], stat_recv.at[layer, q, t],
                          {"tp": lax.rem(t + d, n_tp)}))

        def middle(i, _):
            conv_span(fringe + i * fringe, pl.multiple_of(i * fringe, fringe))
            return 0

        lax.fori_loop(0, chunk // fringe, middle, 0)
        send_stats(0)
        if layer == 0:
            relay(2, 2)
            relay(2, 3)
            detour(2, 0)
        for side_, cond in ((0, s > 0), (1, s < n_sp - 1)):
            guarded(cond, halo_copy(side_).wait_recv)
            to = 0 if side_ == 0 else fringe + rows

            @pl.when(cond)
            def _(side_=side_, to=to):
                wide = halo[layer, side_].astype(F32)
                for j in range(tiles):
                    xbuf[j, pl.ds(to, fringe), :] = wide[:, j * LANES : (j + 1) * LANES]

            @pl.when(jnp.logical_not(cond))
            def _(to=to):
                for j in range(tiles):
                    xbuf[j, pl.ds(to, fringe), :] = jnp.zeros((fringe, LANES), F32)

        def edge(i, _):
            conv_span(i * (rows - fringe), pl.multiple_of(chunk + i * fringe, fringe))
            return 0

        lax.fori_loop(0, 2, edge, 0)
        send_stats(1)
        if layer == 0:
            detour(2, 1)
            detour(2, 2)
        if not last:
            own_x(base_p + 3)
            relay(base_p + 3, 1)
            own_z(base_p + 4)

        def activate(q):
            for d in range(1, n_tp):
                origin = lax.rem(t + n_tp - d, n_tp)
                remote(stat.at[layer, q, t], stat.at[layer, q, origin], stat_send.at[layer, q, d],
                       stat_recv.at[layer, q, origin], {"tp": origin}).wait_recv()
            means = [stat[layer, q, j][0:1] for j in range(n_tp)]
            mean = sum(means) / n_tp
            spread = sum(stat[layer, q, j][1:2] + chan * (means[j] - mean) * (means[j] - mean) for j in range(n_tp))
            scale = lax.rsqrt(spread / (n_tp * chan) + EPSILON)
            row = lax.broadcasted_iota(jnp.int32, (LANES, chunk), 0)
            part[pl.ds(q * chunk, chunk), :] = jnp.transpose(jnp.where(row == 0, mean, scale))

            def act_step(i, _):
                at = pl.ds(pl.multiple_of(q * chunk + i * 32, 32), 32)
                both = part[at, :]
                v = (conv[at, :] - both[:, 0:1]) * both[:, 1:2] * gain_norm[layer : layer + 1, :]
                act[at, :] = (v / (1.0 + jnp.exp(-v))).astype(BF16)
                return 0

            lax.fori_loop(0, chunk // 32, act_step, 0)

        def project(q, target, put):
            for i in range(each):
                block = target * each + i
                pos = lax.rem(block, PAIR) * line + block // PAIR if gather else block
                w = go_w[layer, pos]
                put(slice(i * cols, (i + 1) * cols),
                    jnp.dot(act[pl.ds(q * chunk, chunk), :], w, preferred_element_type=F32))

        def first_copy(q, k):
            return remote(first.at[layer, q, 0, k], first.at[layer, q, 1, k], first_send.at[layer, q, k],
                          first_recv.at[layer, q, k], {"tp": sib})

        def far_copy(q, k, e):
            g = lax.rem(h + e, half)
            return remote(pair.at[layer, q, k], far.at[layer, q, h, k], far_send.at[layer, q, e, k],
                          far_recv.at[layer, q, h, k], {"tp": g * PAIR + c})

        def far_wait(q, k, e):
            g = lax.rem(h + e, half)
            remote(pair.at[layer, q, k], far.at[layer, q, g, k], far_send.at[layer, q, e, k],
                   far_recv.at[layer, q, g, k], {"tp": sib}).wait_recv()

        def last_copy(q, e):
            k = lax.rem(h + e, half)
            return remote(pair.at[layer, q, k], far.at[layer, q, h, 0], far_send.at[layer, q, e, 0],
                          far_recv.at[layer, q, h, 0], {"tp": k * PAIR + c})

        def scatter(q):
            for k in range(half):
                def put_first(cut, v, k=k):
                    first[layer, q, 0, k, :, cut] = v.astype(BF16)

                project(q, k * PAIR + (1 - c), put_first)
                go(first_copy(q, k))
            for k in range(half):
                def put_own(cut, v, k=k):
                    own[k, :, cut] = v

                project(q, k * PAIR + c, put_own)
            for k in range(half):
                first_copy(q, k).wait_recv()
                pair[layer, q, k] = (own[k] + first[layer, q, 1, k].astype(F32)).astype(BF16)
                if not last:
                    for e in range(1, half):
                        go(far_copy(q, k, e))
            if last:
                for e in range(1, half):
                    go(last_copy(q, e))

        def rows_of(q):
            at = 0
            for lo, count in spans[q]:
                yield slice(at, at + count), slice(lo, lo + count)
                at += count

        def gather_stream(q):
            for k in range(half):
                for e in range(1, half):
                    far_wait(q, k, e)
                far[layer, q, h, k] = pair[layer, q, k]
                for src, dst in rows_of(q):
                    total = sum(far[layer, q, g, k, src].astype(F32) for g in range(half))
                    mine = k * PAIR + c
                    stream[layer + 1, mine, dst] = (stream[layer, mine, dst].astype(F32) + total).astype(BF16)
                    i = 0 if dst.start == spans[q][0][0] else 1
                    block = stream.at[layer + 1, mine, dst]
                    go(remote(block, block, sib_send.at[layer, half + 3 * k + q + i], back_recv.at[layer, 3 * k + q + i], {"tp": sib}))

        def gather_wait(q):
            for k in range(half):
                for i, (_, dst) in enumerate(rows_of(q)):
                    block = stream.at[layer + 1, k * PAIR + (1 - c), dst]
                    remote(block, block, sib_send.at[0, 0], back_recv.at[layer, 3 * k + q + i], {"tp": sib}).wait_recv()

        activate(0)
        settle(base_p + 2)
        scatter(0)
        activate(1)
        scatter(1)
        if not last:
            relay(base_p + 3, 2)
            relay(base_p + 3, 3)
            relay(base_p + 4, 1)
            own_x(base_p + 4)
            gather_stream(0)
            relay(base_p + 4, 2)
            relay(base_p + 4, 3)
            detour(base_p + 4, 0)
            detour(base_p + 4, 1)
            detour(base_p + 4, 2)
            own_z(base_p + 5)
            own_x(base_p + 5)
            gather_stream(1)
            relay(base_p + 5, 1)
            relay(base_p + 5, 2)
            relay(base_p + 5, 3)
            gather_wait(0)
            gather_wait(1)
        else:
            for q in range(2):
                far[layer, q, h, 0] = pair[layer, q, h]
                for e in range(1, half):
                    k = lax.rem(h + e, half)
                    remote(pair.at[layer, q, k], far.at[layer, q, k, 0], far_send.at[layer, q, e, 0],
                           far_recv.at[layer, q, k, 0], {"tp": sib}).wait_recv()
                for src, dst in rows_of(q):
                    total = sum(far[layer, q, g, 0, src].astype(F32) for g in range(half))
                    out[dst] = (stream[layer, t, dst].astype(F32) + total).astype(BF16)

    for copy, cond in sends:
        guarded(cond, copy.wait_send)


def per_device(n_sp, n_tp, tokens, segments, in_gain, w_value, w_gate, conv_taps, norm_gain, w_out):
    layers, kw, chan = conv_taps.shape
    rows, width = tokens.shape
    gather = n_sp <= RELAY_MOST and n_sp % PAIR == 0
    if not gather:
        w_value = lax.all_gather(w_value, "sp", axis=1, tiled=True)
        w_gate = lax.all_gather(w_gate, "sp", axis=1, tiled=True)
        w_out = lax.all_gather(w_out, "sp", axis=2, tiled=True)
        w_out = w_out.reshape(layers, chan, n_tp, width).transpose(0, 2, 1, 3)
    held_out = (layers, n_sp) + w_out.shape[1:] if gather else w_out.shape
    tiles, half, fringe = chan // LANES, n_tp // PAIR, (kw - 1) // 2
    wide, chunk = rows + 2 * fringe, rows // 2
    dma = pltpu.SemaphoreType.DMA
    line = n_sp // PAIR
    held_sp = n_sp if gather else 1
    kinds = 3 + 4 * (line - 1) + 2 * line if gather else 1
    hbm = pl.BlockSpec(memory_space=pl.ANY)
    vmem = pl.BlockSpec(memory_space=pltpu.VMEM)
    return pl.pallas_call(
        functools.partial(kernel, (n_sp, n_tp, layers, kw, gather)),
        out_shape=jax.ShapeDtypeStruct((rows, width), BF16),
        in_specs=[hbm] * 8,
        out_specs=vmem,
        scratch_shapes=[
            pltpu.VMEM((layers, n_tp, rows, width), BF16),
            pltpu.VMEM((rows, n_tp * width), BF16),
            pltpu.VMEM((layers, 2, n_tp * width, chan), BF16),
            pltpu.VMEM(held_out, BF16),
            pltpu.VMEM((rows, chan), F32),
            pltpu.VMEM((rows, chan), F32),
            pltpu.VMEM((layers, rows, chan), BF16),
            pltpu.VMEM((layers, 2, fringe, chan), BF16),
            pltpu.VMEM((tiles, wide, LANES), F32),
            pltpu.VMEM((wide, LANES), F32),
            pltpu.VMEM((rows // LANES, LANES), jnp.int32),
            pltpu.VMEM((2, rows // LANES, LANES), jnp.int32),
            pltpu.VMEM((rows, chan), F32),
            pltpu.VMEM((rows, chan), BF16),
            pltpu.VMEM((layers, 2, n_tp, 8, chunk), F32),
            pltpu.VMEM((rows, LANES), F32),
            pltpu.VMEM((layers, 2, 2, half, chunk, width), BF16),
            pltpu.VMEM((layers, 2, half, chunk, width), BF16),
            pltpu.VMEM((layers, 2, half, half, chunk, width), BF16),
            pltpu.VMEM((half, chunk, width), F32),
            pltpu.VMEM(in_gain.shape, F32),
            pltpu.VMEM(norm_gain.shape, F32),
            pltpu.VMEM((kw, layers, chan), F32),
            dma((layers * 3 + 5,)),
            dma((layers * 3, held_sp)),
            dma((layers * 3, kinds)),
            dma((n_tp,)),
            dma((half,)),
            dma((layers, 4 * half)),
            dma((2,)),
            dma((2,)),
            dma((layers, 2)),
            dma((layers, 2)),
            dma((layers, 2, n_tp)),
            dma((layers, 2, n_tp)),
            dma((layers, 2, half)),
            dma((layers, 2, half)),
            dma((layers, 2, half, half)),
            dma((layers, 2, half, half)),
            dma((layers, 3 * half)),
        ],
        compiler_params=pltpu.CompilerParams(
            collective_id=0, has_side_effects=True, vmem_limit_bytes=60000 * 1024
        ),
    )(
        tokens,
        segments.reshape(rows // LANES, LANES),
        in_gain,
        w_value,
        w_gate,
        w_out,
        conv_taps.transpose(1, 0, 2),
        norm_gain,
    )


def solution(mesh):
    in_specs = (
        P("sp", "tp"),
        P("sp"),
        P(),
        P(None, "sp", "tp"),
        P(None, "sp", "tp"),
        P(None, None, "tp"),
        P(None, "tp"),
        P(None, "tp", "sp"),
    )
    return jax.shard_map(
        functools.partial(per_device, mesh.shape["sp"], mesh.shape["tp"]),
        mesh=mesh,
        in_specs=in_specs,
        out_specs=P("sp", "tp"),
        check_vma=False,
    )
```

```python
import functools

import jax
import jax.numpy as jnp
from jax import lax
from jax.experimental import pallas as pl
from jax.experimental.pallas import tpu as pltpu
from jax.sharding import PartitionSpec as P

EPSILON = 0.01
LANES = 128
PAIR = 2
RELAY_MOST = 8
CHAIN = (0, 1)
DETOUR = {3: 2, 5: 1}
PLAN = {
    (0, 11): (("r", 2, 1), ("c", 2, 1), ("z", 3, 0), ("r", 2, 2),),
    (0, 0): (("c", 2, 2),),
    (0, 1): (("r", 2, 3), ("c", 2, 3),),
    (0, 2): (("d", 3, 0), ("z", 4, 0),),
    (0, 4): (("r", 3, 1), ("c", 3, 1), ("r", 3, 2),),
    (0, 5): (("c", 3, 2), ("r", 3, 3), ("c", 3, 3), ("d", 3, 1),),
    (0, 6): (("r", 4, 1), ("c", 4, 1), ("z", 5, 0),),
    (0, 7): (("d", 3, 2), ("r", 4, 2), ("c", 4, 2), ("r", 4, 3), ("c", 4, 3),),
    (1, 0): (("r", 5, 1), ("c", 5, 1), ("d", 5, 0),),
    (1, 1): (("r", 5, 2), ("c", 5, 2),),
    (1, 2): (("r", 5, 3), ("c", 5, 3), ("d", 5, 1),),
    (1, 3): (("d", 5, 2),),
}
F32 = jnp.float32
BF16 = jnp.bfloat16
MESH = pl.DeviceIdType.MESH


def remote(src, dst, send, recv, device):
    return pltpu.make_async_remote_copy(
        src_ref=src, dst_ref=dst, send_sem=send, recv_sem=recv, device_id=device, device_id_type=MESH
    )


def guarded(cond, act):
    if cond is None:
        act()
    else:
        pl.when(cond)(act)


def kernel(
    cfg, tok, seg, gain_in_hbm, wv, wg, wo, taps_hbm, gain_norm_hbm, out,
    stream, normed, gv, go_w, vacc, gacc, gbf, halo, xbuf, segw, segraw, segn, conv, act, stat, part,
    first, pair, far, own, gain_in, gain_norm, taps,
    psend, precv, otok, scl, local_sem, w_recv, w_send, tok_recv, tok_send, sib_send, seg_send, seg_recv,
    halo_send, halo_recv, stat_send, stat_recv, first_send, first_recv, far_send, far_recv, back_recv,
    cross_send, cross_recv, part_send, part_recv,
):
    n_sp, n_tp, layers, kw, gather = cfg
    fringe = (kw - 1) // 2
    rows, width = tok.shape
    tiles = xbuf.shape[0]
    chan = tiles * LANES
    line, half = n_sp // PAIR, n_tp // PAIR
    s, t = lax.axis_index("sp"), lax.axis_index("tp")
    z, x = s // PAIR, lax.rem(s, PAIR)
    h, c = t // PAIR, lax.rem(t, PAIR)
    x_next = z * PAIR + (1 - x)
    sib = h * PAIR + (1 - c)
    mats = 3
    chunk = rows // 2
    depth = min(wv.shape[1], width)
    blocks_in = n_tp * width // depth
    cols = go_w.shape[-1]
    each = width // cols

    sends = []

    def go(copy, cond=None):
        guarded(cond, copy.start)
        sends.append((copy, cond))

    def place(block):
        return (block % PAIR) * line + block // PAIR if gather else block

    def slot(p, zo, xo):
        layer, mat = p // mats, p % mats
        pos = xo * line + zo
        if mat == 2:
            return go_w.at[layer, pos]
        return gv.at[layer, mat, pl.ds(pl.multiple_of(pos * depth, depth), depth)]

    local = []

    def fetch(src, dst):
        copy = pltpu.make_async_copy(src, dst, local_sem.at[len(local)])
        copy.start()
        local.append(copy)
        return copy

    own_copies = []
    for p in range(layers * mats):
        src = (wv, wg, wo)[p % mats].at[p // mats]
        if gather:
            dst = slot(p, z, x)
        else:
            dst = go_w.at[p // mats] if p % mats == 2 else gv.at[p // mats, p % mats]
        own_copies.append((src, dst))
    weight_in = [fetch(*own_copies[0]), fetch(*own_copies[1])]
    tok_in = fetch(tok, stream.at[0, t])
    seg_in = fetch(seg, segraw)
    weight_in += [fetch(*pair_) for pair_ in own_copies[2:]]
    rest_in = [fetch(gain_in_hbm, gain_in), fetch(gain_norm_hbm, gain_norm), fetch(taps_hbm, taps)]

    barrier = pltpu.get_barrier_semaphore()
    prev_s, next_s = jnp.maximum(s - 1, 0), jnp.minimum(s + 1, n_sp - 1)

    def greet(device, cond=None):
        guarded(cond, lambda: pl.semaphore_signal(barrier, inc=1, device_id=device, device_id_type=MESH))

    for d in range(1, n_tp):
        greet({"tp": lax.rem(t + d, n_tp)})
    peers = n_tp - 1
    greet({"sp": prev_s}, s > 0)
    greet({"sp": next_s}, s < n_sp - 1)
    peers = peers + jnp.where(s > 0, 1, 0) + jnp.where(s < n_sp - 1, 1, 0)
    if gather:
        up = {"sp": jnp.minimum(s + PAIR, n_sp - 1)}
        down = {"sp": jnp.maximum(s - PAIR, 0)}
        side = {"sp": x_next}
        up2 = {"sp": jnp.minimum(s + 2 * PAIR, n_sp - 1)}
        down2 = {"sp": jnp.maximum(s - 2 * PAIR, 0)}
        greet(up, z < line - 1)
        greet(down, z > 0)
        greet(up2, z < line - 2)
        greet(down2, z > 1)
        greet(side)
        peers = peers + 1 + jnp.where(z < line - 1, 1, 0) + jnp.where(z > 0, 1, 0)
        peers = peers + jnp.where(z < line - 2, 1, 0) + jnp.where(z > 1, 1, 0)
    pl.semaphore_wait(barrier, peers)

    def push(p, kind, zo, xo, device, cond):
        block = slot(p, zo, xo)
        go(remote(block, block, w_send.at[p, kind], w_recv.at[p, xo * line + zo], device), cond)

    def landed(p, zo, xo, cond):
        block = slot(p, zo, xo)
        guarded(cond, remote(block, block, w_send.at[p, 0], w_recv.at[p, xo * line + zo], {"sp": x_next}).wait_recv)

    def own_z(p):
        if gather:
            push(p, 0, z, x, up, z < line - 1)
            push(p, 1, z, x, down, z > 0)
            if p not in CHAIN:
                k = 3 + 4 * (line - 1) + 2 * line
                push(p, k, z, x, up2, z < line - 2)
                push(p, k + 1, z, x, down2, z > 1)

    def own_x(p):
        if gather:
            push(p, 2, z, x, side, None)

    def sides(d):
        for i, sign in enumerate((1, -1)):
            zo = z - sign * d
            here = (zo >= 0) if sign > 0 else (zo < line)
            yield i, sign, jnp.clip(zo, 0, line - 1), here

    def relay(p, d):
        if d >= line:
            return
        for i, sign, zo, here in sides(d):
            landed(p, zo, x, here)
            onward = (z < line - 1) if sign > 0 else (z > 0)
            if p in CHAIN or d > 1:
                push(p, 3 + i + 4 * (d - 1), zo, x, up if sign > 0 else down, jnp.logical_and(here, onward))

    def across(p, d):
        if d >= line:
            return
        for i, sign, zo, here in sides(d):
            if p in DETOUR:
                here = jnp.logical_and(here, zo != DETOUR[p])
            push(p, 5 + i + 4 * (d - 1), zo, x, side, here)

    def detour(p, d):
        if not gather or p not in DETOUR or d >= line:
            return
        zo = DETOUR[p]
        k = 3 + 4 * (line - 1)
        if d == 0:
            landed(p, zo, 1 - x, z == zo)
            push(p, k, zo, 1 - x, up, jnp.logical_and(z == zo, z < line - 1))
            push(p, k + 1, zo, 1 - x, down, jnp.logical_and(z == zo, z > 0))
        else:
            landed(p, zo, 1 - x, jnp.logical_or(z == zo + d, z == zo - d))
            push(p, k + 2 * d, zo, 1 - x, up, jnp.logical_and(z == zo + d, z < line - 1))
            push(p, k + 2 * d + 1, zo, 1 - x, down, jnp.logical_and(z == zo - d, z > 0))

    def settle(p):
        if not gather or p in CHAIN:
            return
        for d in range(line):
            for sign in ((1,) if d == 0 else (1, -1)):
                zo = z - sign * d
                safe = jnp.clip(zo, 0, line - 1)
                cond = None if d == 0 else ((zo >= 0) if sign > 0 else (zo < line))
                if p in DETOUR:
                    differs = safe != DETOUR[p]
                    cond = differs if cond is None else jnp.logical_and(cond, differs)
                landed(p, safe, 1 - x, cond)

    weight_in[0].wait()
    own_z(0)
    weight_in[1].wait()
    own_z(1)
    tok_in.wait()
    for d in range(1, half):
        go(remote(stream.at[0, t], stream.at[0, t], tok_send.at[d], tok_recv.at[t], {"tp": lax.rem(h + d, half) * PAIR + c}))
    go(remote(stream.at[0, t], stream.at[0, t], sib_send.at[0, 0], tok_recv.at[t], {"tp": sib}))
    if gather:
        theirs = pl.ds(pl.multiple_of((1 - x) * depth, depth), depth)
        go(remote(stream.at[0, t, :, theirs], otok.at[t], cross_send.at[0], cross_recv.at[t], side))
    seg_in.wait()

    def seg_copy(side_):
        return remote(segraw, segn.at[side_], seg_send.at[side_], seg_recv.at[side_], {"sp": prev_s if side_ else next_s})

    go(seg_copy(0), s < n_sp - 1)
    go(seg_copy(1), s > 0)

    def column(row):
        return jnp.transpose(jnp.broadcast_to(row.astype(F32), (LANES, LANES)))

    for i in range(rows // LANES):
        segw[pl.ds(fringe + i * LANES, LANES), :] = column(segraw[i : i + 1, :])

    if gather:
        relay(0, 1)
        relay(1, 1)
    for copy in weight_in[2:] + rest_in:
        copy.wait()
    for d in range(1, half):
        origin = lax.rem(h + half - d, half) * PAIR + c
        block = stream.at[0, origin]
        remote(block, block, tok_send.at[d], tok_recv.at[origin], {"tp": sib}).wait_recv()
        go(remote(block, block, sib_send.at[0, d], tok_recv.at[origin], {"tp": sib}))
    if gather:
        block = otok.at[t]
        remote(block, block, cross_send.at[0], cross_recv.at[t], side).wait_recv()
        for d in range(1, half):
            go(remote(block, block, cross_send.at[d], cross_recv.at[t], {"tp": lax.rem(h + d, half) * PAIR + c}))
        go(remote(block, block, cross_send.at[half], cross_recv.at[t], {"tp": sib}))
        for p in range(2, layers * mats):
            own_x(p)
        relay(0, 2)
        relay(1, 2)
        own_z(2)
        for d in range(1, half):
            origin = lax.rem(h + half - d, half) * PAIR + c
            block = otok.at[origin]
            remote(block, block, cross_send.at[0], cross_recv.at[origin], {"tp": sib}).wait_recv()
            go(remote(block, block, cross_send.at[half + d], cross_recv.at[origin], {"tp": sib}))
        for d in range(half):
            origin = lax.rem(h + half - d, half) * PAIR + (1 - c)
            block = otok.at[origin]
            remote(block, block, cross_send.at[0], cross_recv.at[origin], {"tp": sib}).wait_recv()
    for d in range(half):
        origin = lax.rem(h + half - d, half) * PAIR + (1 - c)
        block = stream.at[0, origin]
        remote(block, block, sib_send.at[0, 0], tok_recv.at[origin], {"tp": sib}).wait_recv()
    guarded(s > 0, seg_copy(0).wait_recv)
    guarded(s < n_sp - 1, seg_copy(1).wait_recv)

    @pl.when(s > 0)
    def _():
        segw[pl.ds(0, fringe), :] = column(segn[0, rows // LANES - 1 : rows // LANES, :])[LANES - fringe :]

    @pl.when(s == 0)
    def _():
        segw[pl.ds(0, fringe), :] = jnp.full((fringe, LANES), -1.0, F32)

    @pl.when(s < n_sp - 1)
    def _():
        segw[pl.ds(fringe + rows, fringe), :] = column(segn[1, 0:1, :])[:fringe]

    @pl.when(s == n_sp - 1)
    def _():
        segw[pl.ds(fringe + rows, fringe), :] = jnp.full((fringe, LANES), -1.0, F32)

    def steps(*names):
        for name in names:
            act_, p, d = name
            {"z": lambda: own_z(p), "x": lambda: own_x(p), "r": lambda: relay(p, d), "c": lambda: across(p, d), "d": lambda: detour(p, d)}[act_]()

    def weigh(layer, point):
        if gather and (layer, point) in PLAN:
            steps(*PLAN[layer, point])

    spans = ((fringe, chunk),), ((0, fringe), (rows - fringe, fringe))

    for layer in range(layers):
        last = layer == layers - 1
        base_p = layer * mats

        def norm_step(i, _):
            at = pl.ds(pl.multiple_of(i * 32, 32), 32)
            total = jnp.zeros((32, 1), F32)
            for j in range(n_tp):
                v = stream[layer, j, at, :].astype(F32)
                total = total + jnp.sum(v * v, axis=-1, keepdims=True)
            scale = lax.rsqrt(total / (n_tp * width) + EPSILON)
            for b in range(blocks_in):
                j, lo = b * depth // width, b * depth % width
                v = stream[layer, j, at, lo : lo + depth].astype(F32)
                gain = gain_in[layer : layer + 1, b * depth : (b + 1) * depth]
                to = place(b) * depth
                normed[at, to : to + depth] = (v * scale * gain).astype(BF16)
            return 0

        size = n_tp * width // 2

        def parity_step(i, _):
            at = pl.ds(pl.multiple_of(i * 32, 32), 32)
            total = jnp.zeros((32, 1), F32)
            for j in range(n_tp):
                v = stream[layer, j, at, :].astype(F32)
                total = total + jnp.sum(v * v, axis=-1, keepdims=True)
                gain = gain_in[layer : layer + 1, pl.ds(pl.multiple_of((2 * j + x) * depth, depth), depth)]
                mine = stream[layer, j, at, pl.ds(pl.multiple_of(x * depth, depth), depth)].astype(F32)
                normed[at, j * depth : (j + 1) * depth] = (mine * gain).astype(BF16)
                other = otok[j, at, :].astype(F32)
                normed[at, size + j * depth : size + (j + 1) * depth] = (other * gain).astype(BF16)
            scl[at, :] = jnp.broadcast_to(lax.rsqrt(total / (n_tp * width) + EPSILON), (32, LANES))
            return 0

        if gather and layer == 0:
            lax.fori_loop(0, rows // 32, parity_step, 0)
            relay(0, 3)
            relay(1, 3)
            near = pl.ds(pl.multiple_of(x * size, size), size)
            for i in range(2):
                at = slice(i * chunk, (i + 1) * chunk)
                for m in range(2):
                    psend[at, m * chan : (m + 1) * chan] = jnp.dot(
                        normed[at, size:], gv[layer, m, near, :], preferred_element_type=F32
                    ).astype(BF16)
                go(remote(psend.at[at], precv.at[at], part_send.at[i], part_recv.at[i], side))
            vacc[...] = jnp.dot(normed[:, :size], gv[layer, 0, near, :], preferred_element_type=F32)
            gacc[...] = jnp.dot(normed[:, :size], gv[layer, 1, near, :], preferred_element_type=F32)
            weigh(layer, 11)
            for i in range(2):
                at = slice(i * chunk, (i + 1) * chunk)
                remote(psend.at[at], precv.at[at], part_send.at[i], part_recv.at[i], side).wait_recv()

            def sum_step(i, _):
                at = pl.ds(pl.multiple_of(i * 32, 32), 32)
                scale = scl[at, 0:1]
                vacc[at, :] = (vacc[at, :] + precv[at, :chan].astype(F32)) * scale
                gacc[at, :] = (gacc[at, :] + precv[at, chan:].astype(F32)) * scale
                return 0

            lax.fori_loop(0, rows // 32, sum_step, 0)
        else:
            lax.fori_loop(0, rows // 32, norm_step, 0)
            near = pl.ds(pl.multiple_of(x * size, size), size) if gather else pl.ds(0, size)
            away = pl.ds(pl.multiple_of((1 - x) * size, size), size) if gather else pl.ds(size, size)
            a = normed[:, near]
            vacc[...] = jnp.dot(a, gv[layer, 0, near, :], preferred_element_type=F32)
            gacc[...] = jnp.dot(a, gv[layer, 1, near, :], preferred_element_type=F32)
            settle(base_p)
            settle(base_p + 1)
            a = normed[:, away]
            vacc[...] += jnp.dot(a, gv[layer, 0, away, :], preferred_element_type=F32)
            gacc[...] += jnp.dot(a, gv[layer, 1, away, :], preferred_element_type=F32)

        def gate_step(i, _):
            at = pl.ds(pl.multiple_of(i * 32, 32), 32)
            gated = (vacc[at, :] * jax.nn.sigmoid(gacc[at, :])).astype(BF16)
            gbf[layer, at, :] = gated
            wide = gated.astype(F32)
            to = pl.ds(pl.multiple_of(fringe + i * 32, 32), 32)
            for j in range(tiles):
                xbuf[j, to, :] = wide[:, j * LANES : (j + 1) * LANES]
            return 0

        lax.fori_loop(0, rows // 32, gate_step, 0)

        def halo_copy(side_):
            lo = 0 if side_ else rows - fringe
            return remote(
                gbf.at[layer, pl.ds(lo, fringe)], halo.at[layer, side_], halo_send.at[layer, side_],
                halo_recv.at[layer, side_], {"sp": prev_s if side_ else next_s},
            )

        go(halo_copy(0), s < n_sp - 1)
        go(halo_copy(1), s > 0)
        weigh(layer, 0)

        def conv_span(start, put):
            base = start
            here = [segw[pl.ds(base + fringe + 8 * m, 8), :] for m in range(8)]
            acc = [[jnp.zeros((8, LANES), F32) for _ in range(tiles)] for _ in range(8)]
            for shift in range(8):
                most = (kw - 1 - shift) // 8
                for n in range(most + 8):
                    at = pl.ds(base + 8 * n + shift, 8)
                    docs = segw[at, :]
                    data = [xbuf[j, at, :] for j in range(tiles)]
                    for m in range(8):
                        if 0 <= n - m <= most:
                            k = 8 * (n - m) + shift
                            same = docs == here[m]
                            for j in range(tiles):
                                tap = taps[k, layer : layer + 1, j * LANES : (j + 1) * LANES]
                                acc[m][j] = acc[m][j] + jnp.where(same, data[j] * tap, 0.0)
            lane = lax.broadcasted_iota(jnp.int32, (8, LANES), 1)
            for m in range(8):
                mean = sum(jnp.sum(v, axis=-1, keepdims=True) for v in acc[m]) / chan
                square = sum(jnp.sum((v - mean) * (v - mean), axis=-1, keepdims=True) for v in acc[m])
                at = pl.ds(put + 8 * m, 8)
                for j in range(tiles):
                    conv[at, j * LANES : (j + 1) * LANES] = acc[m][j]
                part[at, :] = jnp.where(lane == 0, mean, square)

        def send_stats(q):
            stat[layer, q, t] = jnp.transpose(part[pl.ds(q * chunk, chunk), :])[:8]
            for d in range(1, n_tp):
                go(remote(stat.at[layer, q, t], stat.at[layer, q, t], stat_send.at[layer, q, d], stat_recv.at[layer, q, t],
                          {"tp": lax.rem(t + d, n_tp)}))

        for i in range(chunk // fringe):
            conv_span(fringe + i * fringe, i * fringe)
            if i == 0:
                weigh(layer, 1)
        send_stats(0)
        weigh(layer, 2)
        for side_, cond in ((0, s > 0), (1, s < n_sp - 1)):
            guarded(cond, halo_copy(side_).wait_recv)
            to = 0 if side_ == 0 else fringe + rows

            @pl.when(cond)
            def _(side_=side_, to=to):
                wide = halo[layer, side_].astype(F32)
                for j in range(tiles):
                    xbuf[j, pl.ds(to, fringe), :] = wide[:, j * LANES : (j + 1) * LANES]

            @pl.when(jnp.logical_not(cond))
            def _(to=to):
                for j in range(tiles):
                    xbuf[j, pl.ds(to, fringe), :] = jnp.zeros((fringe, LANES), F32)

        for i in range(2):
            conv_span(i * (rows - fringe), chunk + i * fringe)
            if i == 0:
                weigh(layer, 3)
        send_stats(1)
        weigh(layer, 4)

        def activate(q):
            for d in range(1, n_tp):
                origin = lax.rem(t + n_tp - d, n_tp)
                remote(stat.at[layer, q, t], stat.at[layer, q, origin], stat_send.at[layer, q, d],
                       stat_recv.at[layer, q, origin], {"tp": origin}).wait_recv()
            means = [stat[layer, q, j][0:1] for j in range(n_tp)]
            mean = sum(means) / n_tp
            spread = sum(stat[layer, q, j][1:2] + chan * (means[j] - mean) * (means[j] - mean) for j in range(n_tp))
            scale = lax.rsqrt(spread / (n_tp * chan) + EPSILON)
            row = lax.broadcasted_iota(jnp.int32, (LANES, chunk), 0)
            part[pl.ds(q * chunk, chunk), :] = jnp.transpose(jnp.where(row == 0, mean, scale))

            def act_step(i, _):
                at = pl.ds(pl.multiple_of(q * chunk + i * 32, 32), 32)
                both = part[at, :]
                v = (conv[at, :] - both[:, 0:1]) * both[:, 1:2] * gain_norm[layer : layer + 1, :]
                act[at, :] = (v / (1.0 + jnp.exp(-v))).astype(BF16)
                return 0

            lax.fori_loop(0, chunk // 32, act_step, 0)

        def project(q, target, put):
            for i in range(each):
                block = target * each + i
                pos = lax.rem(block, PAIR) * line + block // PAIR if gather else block
                w = go_w[layer, pos]
                put(slice(i * cols, (i + 1) * cols),
                    jnp.dot(act[pl.ds(q * chunk, chunk), :], w, preferred_element_type=F32))

        def first_copy(q, k):
            return remote(first.at[layer, q, 0, k], first.at[layer, q, 1, k], first_send.at[layer, q, k],
                          first_recv.at[layer, q, k], {"tp": sib})

        def far_copy(q, k, e):
            g = lax.rem(h + e, half)
            return remote(pair.at[layer, q, k], far.at[layer, q, h, k], far_send.at[layer, q, e, k],
                          far_recv.at[layer, q, h, k], {"tp": g * PAIR + c})

        def far_wait(q, k, e):
            g = lax.rem(h + e, half)
            remote(pair.at[layer, q, k], far.at[layer, q, g, k], far_send.at[layer, q, e, k],
                   far_recv.at[layer, q, g, k], {"tp": sib}).wait_recv()

        def last_copy(q, e):
            k = lax.rem(h + e, half)
            return remote(pair.at[layer, q, k], far.at[layer, q, h, 0], far_send.at[layer, q, e, 0],
                          far_recv.at[layer, q, h, 0], {"tp": k * PAIR + c})

        def scatter(q):
            for k in range(half):
                def put_first(cut, v, k=k):
                    first[layer, q, 0, k, :, cut] = v.astype(BF16)

                project(q, k * PAIR + (1 - c), put_first)
                go(first_copy(q, k))
            for k in range(half):
                def put_own(cut, v, k=k):
                    own[k, :, cut] = v

                project(q, k * PAIR + c, put_own)
            for k in range(half):
                first_copy(q, k).wait_recv()
                pair[layer, q, k] = (own[k] + first[layer, q, 1, k].astype(F32)).astype(BF16)
                if not last:
                    for e in range(1, half):
                        go(far_copy(q, k, e))
            if last:
                for e in range(1, half):
                    go(last_copy(q, e))

        def rows_of(q):
            at = 0
            for lo, count in spans[q]:
                yield slice(at, at + count), slice(lo, lo + count)
                at += count

        def gather_stream(q):
            for k in range(half):
                for e in range(1, half):
                    far_wait(q, k, e)
                far[layer, q, h, k] = pair[layer, q, k]
                for src, dst in rows_of(q):
                    total = sum(far[layer, q, g, k, src].astype(F32) for g in range(half))
                    mine = k * PAIR + c
                    stream[layer + 1, mine, dst] = (stream[layer, mine, dst].astype(F32) + total).astype(BF16)
                    i = 0 if dst.start == spans[q][0][0] else 1
                    block = stream.at[layer + 1, mine, dst]
                    go(remote(block, block, sib_send.at[layer, half + 3 * k + q + i], back_recv.at[layer, 3 * k + q + i], {"tp": sib}))

        def gather_wait(q):
            for k in range(half):
                for i, (_, dst) in enumerate(rows_of(q)):
                    block = stream.at[layer + 1, k * PAIR + (1 - c), dst]
                    remote(block, block, sib_send.at[0, 0], back_recv.at[layer, 3 * k + q + i], {"tp": sib}).wait_recv()

        activate(0)
        weigh(layer, 10)
        settle(base_p + 2)
        scatter(0)
        weigh(layer, 5)
        activate(1)
        scatter(1)
        weigh(layer, 6)
        if not last:
            gather_stream(0)
            weigh(layer, 7)
            gather_stream(1)
            weigh(layer, 8)
            gather_wait(0)
            gather_wait(1)
        else:
            for q in range(2):
                far[layer, q, h, 0] = pair[layer, q, h]
                for e in range(1, half):
                    k = lax.rem(h + e, half)
                    remote(pair.at[layer, q, k], far.at[layer, q, k, 0], far_send.at[layer, q, e, 0],
                           far_recv.at[layer, q, k, 0], {"tp": sib}).wait_recv()
                for src, dst in rows_of(q):
                    total = sum(far[layer, q, g, 0, src].astype(F32) for g in range(half))
                    out[dst] = (stream[layer, t, dst].astype(F32) + total).astype(BF16)

    for copy, cond in sends:
        guarded(cond, copy.wait_send)


def per_device(n_sp, n_tp, tokens, segments, in_gain, w_value, w_gate, conv_taps, norm_gain, w_out):
    layers, kw, chan = conv_taps.shape
    rows, width = tokens.shape
    gather = n_sp <= RELAY_MOST and n_sp % PAIR == 0
    if not gather:
        w_value = lax.all_gather(w_value, "sp", axis=1, tiled=True)
        w_gate = lax.all_gather(w_gate, "sp", axis=1, tiled=True)
        w_out = lax.all_gather(w_out, "sp", axis=2, tiled=True)
        w_out = w_out.reshape(layers, chan, n_tp, width).transpose(0, 2, 1, 3)
    held_out = (layers, n_sp) + w_out.shape[1:] if gather else w_out.shape
    tiles, half, fringe = chan // LANES, n_tp // PAIR, (kw - 1) // 2
    wide, chunk = rows + 2 * fringe, rows // 2
    dma = pltpu.SemaphoreType.DMA
    line = n_sp // PAIR
    held_sp = n_sp if gather else 1
    kinds = 5 + 4 * (line - 1) + 2 * line if gather else 1
    hbm = pl.BlockSpec(memory_space=pl.ANY)
    vmem = pl.BlockSpec(memory_space=pltpu.VMEM)
    return pl.pallas_call(
        functools.partial(kernel, (n_sp, n_tp, layers, kw, gather)),
        out_shape=jax.ShapeDtypeStruct((rows, width), BF16),
        in_specs=[hbm] * 8,
        out_specs=vmem,
        scratch_shapes=[
            pltpu.VMEM((layers, n_tp, rows, width), BF16),
            pltpu.VMEM((rows, n_tp * width), BF16),
            pltpu.VMEM((layers, 2, n_tp * width, chan), BF16),
            pltpu.VMEM(held_out, BF16),
            pltpu.VMEM((rows, chan), F32),
            pltpu.VMEM((rows, chan), F32),
            pltpu.VMEM((layers, rows, chan), BF16),
            pltpu.VMEM((layers, 2, fringe, chan), BF16),
            pltpu.VMEM((tiles, wide, LANES), F32),
            pltpu.VMEM((wide, LANES), F32),
            pltpu.VMEM((rows // LANES, LANES), jnp.int32),
            pltpu.VMEM((2, rows // LANES, LANES), jnp.int32),
            pltpu.VMEM((rows, chan), F32),
            pltpu.VMEM((rows, chan), BF16),
            pltpu.VMEM((layers, 2, n_tp, 8, chunk), F32),
            pltpu.VMEM((rows, LANES), F32),
            pltpu.VMEM((layers, 2, 2, half, chunk, width), BF16),
            pltpu.VMEM((layers, 2, half, chunk, width), BF16),
            pltpu.VMEM((layers, 2, half, half, chunk, width), BF16),
            pltpu.VMEM((half, chunk, width), F32),
            pltpu.VMEM(in_gain.shape, F32),
            pltpu.VMEM(norm_gain.shape, F32),
            pltpu.VMEM((kw, layers, chan), F32),
            pltpu.VMEM((rows, 2 * chan), BF16),
            pltpu.VMEM((rows, 2 * chan), BF16),
            pltpu.VMEM((n_tp, rows, n_tp * width // n_sp if gather else LANES), BF16),
            pltpu.VMEM((rows, LANES), F32),
            dma((layers * 3 + 5,)),
            dma((layers * 3, held_sp)),
            dma((layers * 3, kinds)),
            dma((n_tp,)),
            dma((half,)),
            dma((layers, 4 * half)),
            dma((2,)),
            dma((2,)),
            dma((layers, 2)),
            dma((layers, 2)),
            dma((layers, 2, n_tp)),
            dma((layers, 2, n_tp)),
            dma((layers, 2, half)),
            dma((layers, 2, half)),
            dma((layers, 2, half, half)),
            dma((layers, 2, half, half)),
            dma((layers, 3 * half)),
            dma((2 * half,)),
            dma((n_tp,)),
            dma((2,)),
            dma((2,)),
        ],
        compiler_params=pltpu.CompilerParams(
            collective_id=0, has_side_effects=True, vmem_limit_bytes=60000 * 1024
        ),
    )(
        tokens,
        segments.reshape(rows // LANES, LANES),
        in_gain,
        w_value,
        w_gate,
        w_out,
        conv_taps.transpose(1, 0, 2),
        norm_gain,
    )


def solution(mesh):
    in_specs = (
        P("sp", "tp"),
        P("sp"),
        P(),
        P(None, "sp", "tp"),
        P(None, "sp", "tp"),
        P(None, None, "tp"),
        P(None, "tp"),
        P(None, "tp", "sp"),
    )
    return jax.shard_map(
        functools.partial(per_device, mesh.shape["sp"], mesh.shape["tp"]),
        mesh=mesh,
        in_specs=in_specs,
        out_specs=P("sp", "tp"),
        check_vma=False,
    )
```

```python
import functools

import jax
import jax.numpy as jnp
from jax import lax
from jax.experimental import pallas as pl
from jax.experimental.pallas import tpu as pltpu
from jax.sharding import PartitionSpec as P

EPSILON = 0.01
LANES = 128
PAIR = 2
RELAY_MOST = 8
CHAIN = (0, 1)
DETOUR = {3: 2, 5: 1}
PLAN = {
    (0, 11): (("r", 2, 1), ("c", 2, 1), ("r", 2, 2), ("z", 3, 0),),
    (0, 0): (("c", 2, 2),),
    (0, 2): (("r", 2, 3), ("c", 2, 3),),
    (0, 3): (("d", 3, 0), ("r", 3, 1), ("c", 3, 1), ("r", 3, 2), ("c", 3, 2), ("z", 4, 0),),
    (0, 6): (("r", 3, 3), ("c", 3, 3), ("d", 3, 1), ("r", 4, 1), ("c", 4, 1), ("d", 3, 2), ("r", 4, 2), ("c", 4, 2), ("z", 5, 0),),
    (0, 7): (("r", 4, 3), ("c", 4, 3),),
    (1, 0): (("r", 5, 1), ("c", 5, 1), ("d", 5, 0),),
    (1, 1): (("r", 5, 2), ("c", 5, 2),),
    (1, 2): (("r", 5, 3), ("c", 5, 3), ("d", 5, 1),),
    (1, 3): (("d", 5, 2),),
}
F32 = jnp.float32
BF16 = jnp.bfloat16
MESH = pl.DeviceIdType.MESH


def remote(src, dst, send, recv, device):
    return pltpu.make_async_remote_copy(
        src_ref=src, dst_ref=dst, send_sem=send, recv_sem=recv, device_id=device, device_id_type=MESH
    )


def guarded(cond, act):
    if cond is None:
        act()
    else:
        pl.when(cond)(act)


def kernel(
    cfg, tok, seg, gain_in_hbm, wv, wg, wo, taps_hbm, gain_norm_hbm, out,
    stream, normed, gv, go_w, vacc, gacc, gbf, halo, xbuf, segw, segraw, segn, conv, act, stat,
    first, pair, far, own, gain_in, gain_norm, taps,
    psend, precv, otok, scl, local_sem, w_recv, w_send, tok_recv, tok_send, sib_send, seg_send, seg_recv,
    halo_send, halo_recv, stat_send, stat_recv, first_send, first_recv, far_send, far_recv, back_recv,
    cross_send, cross_recv, part_send, part_recv,
):
    n_sp, n_tp, layers, kw, gather = cfg
    fringe = (kw - 1) // 2
    rows, width = tok.shape
    tiles = xbuf.shape[0]
    chan = tiles * LANES
    line, half = n_sp // PAIR, n_tp // PAIR
    s, t = lax.axis_index("sp"), lax.axis_index("tp")
    z, x = s // PAIR, lax.rem(s, PAIR)
    h, c = t // PAIR, lax.rem(t, PAIR)
    x_next = z * PAIR + (1 - x)
    sib = h * PAIR + (1 - c)
    mats = 3
    chunk = rows // 2
    depth = min(wv.shape[1], width)
    blocks_in = n_tp * width // depth
    cols = go_w.shape[-1]
    each = width // cols

    sends = []

    def go(copy, cond=None):
        guarded(cond, copy.start)
        sends.append((copy, cond))

    def place(block):
        return (block % PAIR) * line + block // PAIR if gather else block

    def slot(p, zo, xo):
        layer, mat = p // mats, p % mats
        pos = xo * line + zo
        if mat == 2:
            return go_w.at[layer, pos]
        return gv.at[layer, mat, pl.ds(pl.multiple_of(pos * depth, depth), depth)]

    local = []

    def fetch(src, dst):
        copy = pltpu.make_async_copy(src, dst, local_sem.at[len(local)])
        copy.start()
        local.append(copy)
        return copy

    own_copies = []
    for p in range(layers * mats):
        src = (wv, wg, wo)[p % mats].at[p // mats]
        if gather:
            dst = slot(p, z, x)
        else:
            dst = go_w.at[p // mats] if p % mats == 2 else gv.at[p // mats, p % mats]
        own_copies.append((src, dst))
    weight_in = [fetch(*own_copies[0]), fetch(*own_copies[1])]
    tok_in = fetch(tok, stream.at[0, t])
    seg_in = fetch(seg, segraw)
    weight_in += [fetch(*pair_) for pair_ in own_copies[2:]]
    rest_in = [fetch(gain_in_hbm, gain_in), fetch(gain_norm_hbm, gain_norm), fetch(taps_hbm, taps)]

    barrier = pltpu.get_barrier_semaphore()
    prev_s, next_s = jnp.maximum(s - 1, 0), jnp.minimum(s + 1, n_sp - 1)

    def greet(device, cond=None):
        guarded(cond, lambda: pl.semaphore_signal(barrier, inc=1, device_id=device, device_id_type=MESH))

    for d in range(1, n_tp):
        greet({"tp": lax.rem(t + d, n_tp)})
    peers = n_tp - 1
    greet({"sp": prev_s}, s > 0)
    greet({"sp": next_s}, s < n_sp - 1)
    peers = peers + jnp.where(s > 0, 1, 0) + jnp.where(s < n_sp - 1, 1, 0)
    if gather:
        up = {"sp": jnp.minimum(s + PAIR, n_sp - 1)}
        down = {"sp": jnp.maximum(s - PAIR, 0)}
        side = {"sp": x_next}
        up2 = {"sp": jnp.minimum(s + 2 * PAIR, n_sp - 1)}
        down2 = {"sp": jnp.maximum(s - 2 * PAIR, 0)}
        greet(up, z < line - 1)
        greet(down, z > 0)
        greet(up2, z < line - 2)
        greet(down2, z > 1)
        greet(side)
        peers = peers + 1 + jnp.where(z < line - 1, 1, 0) + jnp.where(z > 0, 1, 0)
        peers = peers + jnp.where(z < line - 2, 1, 0) + jnp.where(z > 1, 1, 0)
    pl.semaphore_wait(barrier, peers)

    def push(p, kind, zo, xo, device, cond):
        block = slot(p, zo, xo)
        go(remote(block, block, w_send.at[p, kind], w_recv.at[p, xo * line + zo], device), cond)

    def landed(p, zo, xo, cond):
        block = slot(p, zo, xo)
        guarded(cond, remote(block, block, w_send.at[p, 0], w_recv.at[p, xo * line + zo], {"sp": x_next}).wait_recv)

    def own_z(p):
        if gather:
            push(p, 0, z, x, up, z < line - 1)
            push(p, 1, z, x, down, z > 0)
            if p not in CHAIN:
                k = 3 + 4 * (line - 1) + 2 * line
                push(p, k, z, x, up2, z < line - 2)
                push(p, k + 1, z, x, down2, z > 1)

    def own_x(p):
        if gather:
            push(p, 2, z, x, side, None)

    def sides(d):
        for i, sign in enumerate((1, -1)):
            zo = z - sign * d
            here = (zo >= 0) if sign > 0 else (zo < line)
            yield i, sign, jnp.clip(zo, 0, line - 1), here

    def relay(p, d):
        if d >= line:
            return
        for i, sign, zo, here in sides(d):
            landed(p, zo, x, here)
            onward = (z < line - 1) if sign > 0 else (z > 0)
            if p in CHAIN or d > 1:
                push(p, 3 + i + 4 * (d - 1), zo, x, up if sign > 0 else down, jnp.logical_and(here, onward))

    def across(p, d):
        if d >= line:
            return
        for i, sign, zo, here in sides(d):
            if p in DETOUR:
                here = jnp.logical_and(here, zo != DETOUR[p])
            push(p, 5 + i + 4 * (d - 1), zo, x, side, here)

    def detour(p, d):
        if not gather or p not in DETOUR or d >= line:
            return
        zo = DETOUR[p]
        k = 3 + 4 * (line - 1)
        if d == 0:
            landed(p, zo, 1 - x, z == zo)
            push(p, k, zo, 1 - x, up, jnp.logical_and(z == zo, z < line - 1))
            push(p, k + 1, zo, 1 - x, down, jnp.logical_and(z == zo, z > 0))
        else:
            landed(p, zo, 1 - x, jnp.logical_or(z == zo + d, z == zo - d))
            push(p, k + 2 * d, zo, 1 - x, up, jnp.logical_and(z == zo + d, z < line - 1))
            push(p, k + 2 * d + 1, zo, 1 - x, down, jnp.logical_and(z == zo - d, z > 0))

    def settle(p):
        if not gather or p in CHAIN:
            return
        for d in range(line):
            for sign in ((1,) if d == 0 else (1, -1)):
                zo = z - sign * d
                safe = jnp.clip(zo, 0, line - 1)
                cond = None if d == 0 else ((zo >= 0) if sign > 0 else (zo < line))
                if p in DETOUR:
                    differs = safe != DETOUR[p]
                    cond = differs if cond is None else jnp.logical_and(cond, differs)
                landed(p, safe, 1 - x, cond)

    weight_in[0].wait()
    own_z(0)
    weight_in[1].wait()
    own_z(1)
    tok_in.wait()
    for d in range(1, half):
        go(remote(stream.at[0, t], stream.at[0, t], tok_send.at[d], tok_recv.at[t], {"tp": lax.rem(h + d, half) * PAIR + c}))
    go(remote(stream.at[0, t], stream.at[0, t], sib_send.at[0, 0], tok_recv.at[t], {"tp": sib}))
    if gather:
        theirs = pl.ds(pl.multiple_of((1 - x) * depth, depth), depth)
        go(remote(stream.at[0, t, :, theirs], otok.at[t], cross_send.at[0], cross_recv.at[t], side))
    seg_in.wait()

    def seg_copy(side_):
        return remote(segraw, segn.at[side_], seg_send.at[side_], seg_recv.at[side_], {"sp": prev_s if side_ else next_s})

    go(seg_copy(0), s < n_sp - 1)
    go(seg_copy(1), s > 0)

    def column(row):
        return jnp.transpose(jnp.broadcast_to(row.astype(F32), (LANES, LANES)))

    for i in range(rows // LANES):
        segw[pl.ds(fringe + i * LANES, LANES), :] = column(segraw[i : i + 1, :])

    if gather:
        relay(0, 1)
        relay(1, 1)
    for copy in weight_in[2:] + rest_in:
        copy.wait()
    for d in range(1, half):
        origin = lax.rem(h + half - d, half) * PAIR + c
        block = stream.at[0, origin]
        remote(block, block, tok_send.at[d], tok_recv.at[origin], {"tp": sib}).wait_recv()
        go(remote(block, block, sib_send.at[0, d], tok_recv.at[origin], {"tp": sib}))
    if gather:
        block = otok.at[t]
        remote(block, block, cross_send.at[0], cross_recv.at[t], side).wait_recv()
        for d in range(1, half):
            go(remote(block, block, cross_send.at[d], cross_recv.at[t], {"tp": lax.rem(h + d, half) * PAIR + c}))
        go(remote(block, block, cross_send.at[half], cross_recv.at[t], {"tp": sib}))
        for p in range(2, layers * mats):
            own_x(p)
        relay(0, 2)
        relay(1, 2)
        own_z(2)
        for d in range(1, half):
            origin = lax.rem(h + half - d, half) * PAIR + c
            block = otok.at[origin]
            remote(block, block, cross_send.at[0], cross_recv.at[origin], {"tp": sib}).wait_recv()
            go(remote(block, block, cross_send.at[half + d], cross_recv.at[origin], {"tp": sib}))
        for d in range(half):
            origin = lax.rem(h + half - d, half) * PAIR + (1 - c)
            block = otok.at[origin]
            remote(block, block, cross_send.at[0], cross_recv.at[origin], {"tp": sib}).wait_recv()
    for d in range(half):
        origin = lax.rem(h + half - d, half) * PAIR + (1 - c)
        block = stream.at[0, origin]
        remote(block, block, sib_send.at[0, 0], tok_recv.at[origin], {"tp": sib}).wait_recv()
    guarded(s > 0, seg_copy(0).wait_recv)
    guarded(s < n_sp - 1, seg_copy(1).wait_recv)

    @pl.when(s > 0)
    def _():
        segw[pl.ds(0, fringe), :] = column(segn[0, rows // LANES - 1 : rows // LANES, :])[LANES - fringe :]

    @pl.when(s == 0)
    def _():
        segw[pl.ds(0, fringe), :] = jnp.full((fringe, LANES), -1.0, F32)

    @pl.when(s < n_sp - 1)
    def _():
        segw[pl.ds(fringe + rows, fringe), :] = column(segn[1, 0:1, :])[:fringe]

    @pl.when(s == n_sp - 1)
    def _():
        segw[pl.ds(fringe + rows, fringe), :] = jnp.full((fringe, LANES), -1.0, F32)

    def steps(*names):
        for name in names:
            act_, p, d = name
            {"z": lambda: own_z(p), "x": lambda: own_x(p), "r": lambda: relay(p, d), "c": lambda: across(p, d), "d": lambda: detour(p, d)}[act_]()

    def weigh(layer, point):
        if gather and (layer, point) in PLAN:
            steps(*PLAN[layer, point])

    spans = ((fringe, chunk),), ((0, fringe), (rows - fringe, fringe))

    for layer in range(layers):
        last = layer == layers - 1
        base_p = layer * mats

        def norm_step(i, _):
            at = pl.ds(pl.multiple_of(i * 32, 32), 32)
            total = jnp.zeros((32, 1), F32)
            for j in range(n_tp):
                v = stream[layer, j, at, :].astype(F32)
                total = total + jnp.sum(v * v, axis=-1, keepdims=True)
            scale = lax.rsqrt(total / (n_tp * width) + EPSILON)
            for b in range(blocks_in):
                j, lo = b * depth // width, b * depth % width
                v = stream[layer, j, at, lo : lo + depth].astype(F32)
                gain = gain_in[layer : layer + 1, b * depth : (b + 1) * depth]
                to = place(b) * depth
                normed[at, to : to + depth] = (v * scale * gain).astype(BF16)
            return 0

        size = n_tp * width // 2

        def parity_step(i, _):
            at = pl.ds(pl.multiple_of(i * 32, 32), 32)
            total = jnp.zeros((32, 1), F32)
            for j in range(n_tp):
                v = stream[layer, j, at, :].astype(F32)
                total = total + jnp.sum(v * v, axis=-1, keepdims=True)
                gain = gain_in[layer : layer + 1, pl.ds(pl.multiple_of((2 * j + x) * depth, depth), depth)]
                mine = stream[layer, j, at, pl.ds(pl.multiple_of(x * depth, depth), depth)].astype(F32)
                normed[at, j * depth : (j + 1) * depth] = (mine * gain).astype(BF16)
                other = otok[j, at, :].astype(F32)
                normed[at, size + j * depth : size + (j + 1) * depth] = (other * gain).astype(BF16)
            scl[at, :] = jnp.broadcast_to(lax.rsqrt(total / (n_tp * width) + EPSILON), (32, LANES))
            return 0

        if gather and layer == 0:
            lax.fori_loop(0, rows // 32, parity_step, 0)
            relay(0, 3)
            relay(1, 3)
            near = pl.ds(pl.multiple_of(x * size, size), size)
            for i in range(2):
                at = slice(i * chunk, (i + 1) * chunk)
                for m in range(2):
                    psend[at, m * chan : (m + 1) * chan] = jnp.dot(
                        normed[at, size:], gv[layer, m, near, :], preferred_element_type=F32
                    ).astype(BF16)
                go(remote(psend.at[at], precv.at[at], part_send.at[i], part_recv.at[i], side))
            vacc[...] = jnp.dot(normed[:, :size], gv[layer, 0, near, :], preferred_element_type=F32)
            gacc[...] = jnp.dot(normed[:, :size], gv[layer, 1, near, :], preferred_element_type=F32)
            weigh(layer, 11)
            for i in range(2):
                at = slice(i * chunk, (i + 1) * chunk)
                remote(psend.at[at], precv.at[at], part_send.at[i], part_recv.at[i], side).wait_recv()

            def sum_step(i, _):
                at = pl.ds(pl.multiple_of(i * 32, 32), 32)
                scale = scl[at, 0:1]
                vacc[at, :] = (vacc[at, :] + precv[at, :chan].astype(F32)) * scale
                gacc[at, :] = (gacc[at, :] + precv[at, chan:].astype(F32)) * scale
                return 0

            lax.fori_loop(0, rows // 32, sum_step, 0, unroll=4)
        else:
            lax.fori_loop(0, rows // 32, norm_step, 0, unroll=4)
            near = pl.ds(pl.multiple_of(x * size, size), size) if gather else pl.ds(0, size)
            away = pl.ds(pl.multiple_of((1 - x) * size, size), size) if gather else pl.ds(size, size)
            a = normed[:, near]
            vacc[...] = jnp.dot(a, gv[layer, 0, near, :], preferred_element_type=F32)
            gacc[...] = jnp.dot(a, gv[layer, 1, near, :], preferred_element_type=F32)
            settle(base_p)
            settle(base_p + 1)
            a = normed[:, away]
            vacc[...] += jnp.dot(a, gv[layer, 0, away, :], preferred_element_type=F32)
            gacc[...] += jnp.dot(a, gv[layer, 1, away, :], preferred_element_type=F32)

        def gate_step(i, _):
            at = pl.ds(pl.multiple_of(i * 32, 32), 32)
            gated = (vacc[at, :] * jax.nn.sigmoid(gacc[at, :])).astype(BF16)
            gbf[layer, at, :] = gated
            wide = gated.astype(F32)
            to = pl.ds(pl.multiple_of(fringe + i * 32, 32), 32)
            for j in range(tiles):
                xbuf[j, to, :] = wide[:, j * LANES : (j + 1) * LANES]
            return 0

        lax.fori_loop(0, rows // 32, gate_step, 0, unroll=2)

        def halo_copy(side_):
            lo = 0 if side_ else rows - fringe
            return remote(
                gbf.at[layer, pl.ds(lo, fringe)], halo.at[layer, side_], halo_send.at[layer, side_],
                halo_recv.at[layer, side_], {"sp": prev_s if side_ else next_s},
            )

        go(halo_copy(0), s < n_sp - 1)
        go(halo_copy(1), s > 0)
        weigh(layer, 0)

        def conv_span(start, put):
            base = start
            here = [segw[pl.ds(base + fringe + 8 * m, 8), :] for m in range(8)]
            acc = [[jnp.zeros((8, LANES), F32) for _ in range(tiles)] for _ in range(8)]
            for shift in range(8):
                most = (kw - 1 - shift) // 8
                for n in range(most + 8):
                    at = pl.ds(base + 8 * n + shift, 8)
                    docs = segw[at, :]
                    data = [xbuf[j, at, :] for j in range(tiles)]
                    for m in range(8):
                        if 0 <= n - m <= most:
                            k = 8 * (n - m) + shift
                            same = docs == here[m]
                            for j in range(tiles):
                                tap = taps[k, layer : layer + 1, j * LANES : (j + 1) * LANES]
                                acc[m][j] = acc[m][j] + jnp.where(same, data[j] * tap, 0.0)
            for m in range(8):
                for j in range(tiles):
                    conv[pl.ds(put + 8 * m, 8), j * LANES : (j + 1) * LANES] = acc[m][j]

        def send_stats(q):
            at = slice(q * chunk, (q + 1) * chunk)
            mean = jnp.sum(conv[at, :], axis=-1, keepdims=True) / chan
            square = jnp.sum((conv[at, :] - mean) * (conv[at, :] - mean), axis=-1, keepdims=True)
            lane = lax.broadcasted_iota(jnp.int32, (chunk, LANES), 1)
            stat[layer, q, t] = jnp.transpose(jnp.where(lane == 0, mean, square))[:8]
            for d in range(1, n_tp):
                go(remote(stat.at[layer, q, t], stat.at[layer, q, t], stat_send.at[layer, q, d], stat_recv.at[layer, q, t],
                          {"tp": lax.rem(t + d, n_tp)}))

        for i in range(chunk // fringe):
            conv_span(fringe + i * fringe, i * fringe)
            if i == 0:
                weigh(layer, 1)
        send_stats(0)
        weigh(layer, 2)
        for side_, cond in ((0, s > 0), (1, s < n_sp - 1)):
            guarded(cond, halo_copy(side_).wait_recv)
            to = 0 if side_ == 0 else fringe + rows

            @pl.when(cond)
            def _(side_=side_, to=to):
                wide = halo[layer, side_].astype(F32)
                for j in range(tiles):
                    xbuf[j, pl.ds(to, fringe), :] = wide[:, j * LANES : (j + 1) * LANES]

            @pl.when(jnp.logical_not(cond))
            def _(to=to):
                for j in range(tiles):
                    xbuf[j, pl.ds(to, fringe), :] = jnp.zeros((fringe, LANES), F32)

        for i in range(2):
            conv_span(i * (rows - fringe), chunk + i * fringe)
            if i == 0:
                weigh(layer, 3)
        send_stats(1)
        weigh(layer, 4)

        def activate(q):
            for d in range(1, n_tp):
                origin = lax.rem(t + n_tp - d, n_tp)
                remote(stat.at[layer, q, t], stat.at[layer, q, origin], stat_send.at[layer, q, d],
                       stat_recv.at[layer, q, origin], {"tp": origin}).wait_recv()
            means = [stat[layer, q, j][0:1] for j in range(n_tp)]
            mean = sum(means) / n_tp
            spread = sum(stat[layer, q, j][1:2] + chan * (means[j] - mean) * (means[j] - mean) for j in range(n_tp))
            scale = lax.rsqrt(spread / (n_tp * chan) + EPSILON)
            row = lax.broadcasted_iota(jnp.int32, (LANES, chunk), 0)
            both = jnp.transpose(jnp.where(row == 0, mean, scale))
            for i in range(chunk // fringe):
                at = slice(q * chunk + i * fringe, q * chunk + (i + 1) * fringe)
                cut = both[i * fringe : (i + 1) * fringe]
                v = (conv[at, :] - cut[:, 0:1]) * cut[:, 1:2] * gain_norm[layer : layer + 1, :]
                act[at, :] = (v / (1.0 + jnp.exp(-v))).astype(BF16)

        def project(q, target, put):
            for i in range(each):
                block = target * each + i
                pos = lax.rem(block, PAIR) * line + block // PAIR if gather else block
                w = go_w[layer, pos]
                put(slice(i * cols, (i + 1) * cols),
                    jnp.dot(act[pl.ds(q * chunk, chunk), :], w, preferred_element_type=F32))

        def first_copy(q, k):
            return remote(first.at[layer, q, 0, k], first.at[layer, q, 1, k], first_send.at[layer, q, k],
                          first_recv.at[layer, q, k], {"tp": sib})

        def far_copy(q, k, e):
            g = lax.rem(h + e, half)
            return remote(pair.at[layer, q, k], far.at[layer, q, h, k], far_send.at[layer, q, e, k],
                          far_recv.at[layer, q, h, k], {"tp": g * PAIR + c})

        def far_wait(q, k, e):
            g = lax.rem(h + e, half)
            remote(pair.at[layer, q, k], far.at[layer, q, g, k], far_send.at[layer, q, e, k],
                   far_recv.at[layer, q, g, k], {"tp": sib}).wait_recv()

        def last_copy(q, e):
            k = lax.rem(h + e, half)
            return remote(pair.at[layer, q, k], far.at[layer, q, h, 0], far_send.at[layer, q, e, 0],
                          far_recv.at[layer, q, h, 0], {"tp": k * PAIR + c})

        def scatter(q):
            order = [lax.rem(h + 1 + i, half) for i in range(half)] if last else list(range(half))
            for k in order:
                def put_first(cut, v, k=k):
                    first[layer, q, 0, k, :, cut] = v.astype(BF16)

                project(q, k * PAIR + (1 - c), put_first)
                go(first_copy(q, k))
            for i, k in enumerate(order):
                def put_own(cut, v, i=i):
                    own[i, :, cut] = v

                project(q, k * PAIR + c, put_own)
                first_copy(q, k).wait_recv()
                pair[layer, q, k] = (own[i] + first[layer, q, 1, k].astype(F32)).astype(BF16)
                if not last:
                    for e in range(1, half):
                        go(far_copy(q, k, e))
                elif i < half - 1:
                    go(last_copy(q, i + 1))

        def rows_of(q):
            at = 0
            for lo, count in spans[q]:
                yield slice(at, at + count), slice(lo, lo + count)
                at += count

        def gather_stream(q):
            for k in range(half):
                for e in range(1, half):
                    far_wait(q, k, e)
                far[layer, q, h, k] = pair[layer, q, k]
                for src, dst in rows_of(q):
                    total = sum(far[layer, q, g, k, src].astype(F32) for g in range(half))
                    mine = k * PAIR + c
                    stream[layer + 1, mine, dst] = (stream[layer, mine, dst].astype(F32) + total).astype(BF16)
                    i = 0 if dst.start == spans[q][0][0] else 1
                    block = stream.at[layer + 1, mine, dst]
                    go(remote(block, block, sib_send.at[layer, half + 3 * k + q + i], back_recv.at[layer, 3 * k + q + i], {"tp": sib}))

        def gather_wait(q):
            for k in range(half):
                for i, (_, dst) in enumerate(rows_of(q)):
                    block = stream.at[layer + 1, k * PAIR + (1 - c), dst]
                    remote(block, block, sib_send.at[0, 0], back_recv.at[layer, 3 * k + q + i], {"tp": sib}).wait_recv()

        activate(0)
        weigh(layer, 10)
        settle(base_p + 2)
        scatter(0)
        weigh(layer, 5)
        activate(1)
        scatter(1)
        weigh(layer, 6)
        if not last:
            gather_stream(0)
            weigh(layer, 7)
            gather_stream(1)
            weigh(layer, 8)
            gather_wait(0)
            gather_wait(1)
        else:
            for q in range(2):
                far[layer, q, h, 0] = pair[layer, q, h]
                for e in range(1, half):
                    k = lax.rem(h + e, half)
                    remote(pair.at[layer, q, k], far.at[layer, q, k, 0], far_send.at[layer, q, e, 0],
                           far_recv.at[layer, q, k, 0], {"tp": sib}).wait_recv()
                for src, dst in rows_of(q):
                    total = sum(far[layer, q, g, 0, src].astype(F32) for g in range(half))
                    out[dst] = (stream[layer, t, dst].astype(F32) + total).astype(BF16)

    for copy, cond in sends:
        guarded(cond, copy.wait_send)


def per_device(n_sp, n_tp, tokens, segments, in_gain, w_value, w_gate, conv_taps, norm_gain, w_out):
    layers, kw, chan = conv_taps.shape
    rows, width = tokens.shape
    gather = n_sp <= RELAY_MOST and n_sp % PAIR == 0
    if not gather:
        w_value = lax.all_gather(w_value, "sp", axis=1, tiled=True)
        w_gate = lax.all_gather(w_gate, "sp", axis=1, tiled=True)
        w_out = lax.all_gather(w_out, "sp", axis=2, tiled=True)
        w_out = w_out.reshape(layers, chan, n_tp, width).transpose(0, 2, 1, 3)
    held_out = (layers, n_sp) + w_out.shape[1:] if gather else w_out.shape
    tiles, half, fringe = chan // LANES, n_tp // PAIR, (kw - 1) // 2
    wide, chunk = rows + 2 * fringe, rows // 2
    dma = pltpu.SemaphoreType.DMA
    line = n_sp // PAIR
    held_sp = n_sp if gather else 1
    kinds = 5 + 4 * (line - 1) + 2 * line if gather else 1
    hbm = pl.BlockSpec(memory_space=pl.ANY)
    vmem = pl.BlockSpec(memory_space=pltpu.VMEM)
    return pl.pallas_call(
        functools.partial(kernel, (n_sp, n_tp, layers, kw, gather)),
        out_shape=jax.ShapeDtypeStruct((rows, width), BF16),
        in_specs=[hbm] * 8,
        out_specs=vmem,
        scratch_shapes=[
            pltpu.VMEM((layers, n_tp, rows, width), BF16),
            pltpu.VMEM((rows, n_tp * width), BF16),
            pltpu.VMEM((layers, 2, n_tp * width, chan), BF16),
            pltpu.VMEM(held_out, BF16),
            pltpu.VMEM((rows, chan), F32),
            pltpu.VMEM((rows, chan), F32),
            pltpu.VMEM((layers, rows, chan), BF16),
            pltpu.VMEM((layers, 2, fringe, chan), BF16),
            pltpu.VMEM((tiles, wide, LANES), F32),
            pltpu.VMEM((wide, LANES), F32),
            pltpu.VMEM((rows // LANES, LANES), jnp.int32),
            pltpu.VMEM((2, rows // LANES, LANES), jnp.int32),
            pltpu.VMEM((rows, chan), F32),
            pltpu.VMEM((rows, chan), BF16),
            pltpu.VMEM((layers, 2, n_tp, 8, chunk), F32),
            pltpu.VMEM((layers, 2, 2, half, chunk, width), BF16),
            pltpu.VMEM((layers, 2, half, chunk, width), BF16),
            pltpu.VMEM((layers, 2, half, half, chunk, width), BF16),
            pltpu.VMEM((half, chunk, width), F32),
            pltpu.VMEM(in_gain.shape, F32),
            pltpu.VMEM(norm_gain.shape, F32),
            pltpu.VMEM((kw, layers, chan), F32),
            pltpu.VMEM((rows, 2 * chan), BF16),
            pltpu.VMEM((rows, 2 * chan), BF16),
            pltpu.VMEM((n_tp, rows, n_tp * width // n_sp if gather else LANES), BF16),
            pltpu.VMEM((rows, LANES), F32),
            dma((layers * 3 + 5,)),
            dma((layers * 3, held_sp)),
            dma((layers * 3, kinds)),
            dma((n_tp,)),
            dma((half,)),
            dma((layers, 4 * half)),
            dma((2,)),
            dma((2,)),
            dma((layers, 2)),
            dma((layers, 2)),
            dma((layers, 2, n_tp)),
            dma((layers, 2, n_tp)),
            dma((layers, 2, half)),
            dma((layers, 2, half)),
            dma((layers, 2, half, half)),
            dma((layers, 2, half, half)),
            dma((layers, 3 * half)),
            dma((2 * half,)),
            dma((n_tp,)),
            dma((2,)),
            dma((2,)),
        ],
        compiler_params=pltpu.CompilerParams(
            collective_id=0, has_side_effects=True, vmem_limit_bytes=60000 * 1024
        ),
    )(
        tokens,
        segments.reshape(rows // LANES, LANES),
        in_gain,
        w_value,
        w_gate,
        w_out,
        conv_taps.transpose(1, 0, 2),
        norm_gain,
    )


def solution(mesh):
    in_specs = (
        P("sp", "tp"),
        P("sp"),
        P(),
        P(None, "sp", "tp"),
        P(None, "sp", "tp"),
        P(None, None, "tp"),
        P(None, "tp"),
        P(None, "tp", "sp"),
    )
    return jax.shard_map(
        functools.partial(per_device, mesh.shape["sp"], mesh.shape["tp"]),
        mesh=mesh,
        in_specs=in_specs,
        out_specs=P("sp", "tp"),
        check_vma=False,
    )
```
